32 devices in a mesh: fs: 8 (over z, x), tp: 4 (over y, core).
Axes of the slice: x: 2, y: 2, z: 4, core: 2. Of those that a mesh axis runs over, the one named last changes fastest.
Arguments:
- query_rows: bfloat16 [16384, 2048], P('fs', 'tp'), may hold values from -16 to 16
- key_rows: bfloat16 [16384, 2048], P('fs', 'tp'), may hold values from -8 to 8
- value_rows: bfloat16 [16384, 2048], P('fs', 'tp'), may hold values from -6 to 6
- mix_lambda: float32 [16], P('tp'), may hold values from 0.3 to 0.8
- head_gain: float32 [128], replicated, may hold values from 0.1 to 1.9
- out_cotangent: bfloat16 [16384, 2048], P('fs'), may hold values from -0.049804688 to 0.049804688
- layer_input: bfloat16 [16384, 2048], P('fs'), may hold values from -6 to 6
- value_cotangent: bfloat16 [16384, 2048], P('fs', 'tp'), may hold values from -0.049804688 to 0.049804688
- out_weight: float32 [2048, 2048], P('tp', 'fs'), may hold values from -0.125 to 0.125
- value_weight: float32 [2048, 2048], P('fs', 'tp'), may hold values from -0.125 to 0.125
- out_basis: bfloat16 [2048, 256], replicated, may hold values from -0.125 to 0.125
- value_basis: bfloat16 [2048, 256], replicated, may hold values from -0.125 to 0.125
- out_first: float32 [256, 2048], P('fs', 'tp'), may hold values from -20 to 20
- out_second: float32 [256, 2048], P('fs', 'tp'), may hold values from 0.02 to 0.5
- value_first: float32 [256, 2048], P('fs', 'tp'), may hold values from -20 to 20
- value_second: float32 [256, 2048], P('fs', 'tp'), may hold values from 0.02 to 0.5
Outputs:
- out_step: float32 [2048, 2048], P('tp', 'fs')
- value_step: float32 [2048, 2048], P('fs', 'tp')
- new_out_weight: float32 [2048, 2048], P('tp', 'fs')
- new_value_weight: float32 [2048, 2048], P('fs', 'tp')
- out_copy: bfloat16 [2048, 2048], P('tp')
- value_copy: bfloat16 [2048, 2048], P(None, 'tp')
- new_out_first: float32 [256, 2048], P('fs', 'tp')
- new_out_second: float32 [256, 2048], P('fs', 'tp')
- new_value_first: float32 [256, 2048], P('fs', 'tp')
- new_value_second: float32 [256, 2048], P('fs', 'tp')
The draws below stay inside these ranges and needn't reach their ends.
All inputs are finite; a program needn't handle non-finite values.
Results may differ from the reference program's by a relative error of at most 0.001.
Values may be sent and summed in bfloat16 or wider, within the bound.
A program may use at most 192 MiB of HBM per device.

```python
import math
import jax
import jax.numpy as jnp
from jax import lax

D = 2048
H = 16
DH = 64
DV = 128
RANK = 256
LEN = 2048
TOKENS = 16384
V = 2048
QKW = 2048


def draw_query_rows(key, part):
    base_draw = jnp.clip(jax.random.normal(jax.random.fold_in(key, 1), (TOKENS // LEN, LEN, 2 * H, DH), jnp.float32) * 1.3, -5.2, 5.2)
    return jnp.clip(base_draw, -16.0, 16.0).reshape(TOKENS, QKW).astype(jnp.bfloat16)


def draw_key_rows(key, part):
    base_draw = jnp.clip(jax.random.normal(jax.random.fold_in(key, 2), (TOKENS // LEN, LEN, 2 * H, DH), jnp.float32) * 1.3, -5.2, 5.2)
    return jnp.clip(base_draw, -8.0, 8.0).reshape(TOKENS, QKW).astype(jnp.bfloat16)


def moment_draw(key, salt):
    row_rise = jnp.arange(RANK, dtype=jnp.float32)[:, None] / RANK
    col_rise = jnp.arange(V, dtype=jnp.float32)[None, :] / V
    jitter = jax.random.uniform(jax.random.fold_in(key, salt), (RANK, V), jnp.float32, -0.35, 0.35)
    scales = 0.3 * 10.0 ** (0.5 * (row_rise + col_rise)) * jnp.exp(jitter)
    values = jnp.clip(jax.random.normal(jax.random.fold_in(key, salt + 1), (RANK, V), jnp.float32), -4.0, 4.0)
    return jnp.clip(values * scales, -20.0, 20.0)


def draw_out_first(key, part):
    return moment_draw(key, 11)


def draw_value_first(key, part):
    return moment_draw(key, 21)


def shard_levels(key, shape, split, least, top_value):
    level = 1.0
    for axis_at, parts in split:
        heights = jax.random.uniform(jax.random.fold_in(jax.random.fold_in(key, 6), axis_at), (parts,), jnp.float32, least / len(split), top_value / len(split))
        level = level * jnp.repeat(jnp.exp(heights), shape[axis_at] // parts).reshape((-1,) + (1,) * (len(shape) - 1 - axis_at))
    return level


def scatter_about(key, shape, spread, reach, pieces=(), kind=jnp.bfloat16):
    drawn = jax.random.normal(key, shape, jnp.float32) * spread
    if len(pieces) > 0:
        drawn = shard_levels(key, shape, pieces, -0.22, 0.18) * drawn
    return jnp.clip(drawn, min=-reach, max=reach).astype(kind)


def setup_inputs(seed: int = 0) -> dict:
    key_list = jax.random.split(jax.random.key(seed), 17)
    return {
        "query_rows": draw_query_rows(jax.random.fold_in(key_list[16], 71), 0),
        "key_rows": draw_key_rows(jax.random.fold_in(key_list[16], 71), 0),
        "value_rows": scatter_about(key_list[2], (TOKENS, V), 1.0, 6.0, ((0, 8), (1, 4))),
        "mix_lambda": jnp.clip(0.3 + 0.5 * jax.random.uniform(key_list[3], (H,), jnp.float32) ** shard_levels(key_list[3], (H,), ((0, 4),), -0.2, 0.2), 0.3, 0.8),
        "head_gain": jnp.clip(1.0 + 0.18 * jax.random.normal(key_list[4], (DV,), jnp.float32), 0.1, 1.9),
        "out_cotangent": scatter_about(key_list[5], (TOKENS, D), 0.008, 0.049804688, ((0, 8),)),
        "layer_input": scatter_about(key_list[6], (TOKENS, D), 1.0, 6.0, ((0, 8),)),
        "value_cotangent": scatter_about(key_list[7], (TOKENS, V), 0.008, 0.049804688, ((0, 8), (1, 4))),
        "out_weight": scatter_about(key_list[8], (V, D), V ** -0.5, 0.125, ((0, 4), (1, 8)), jnp.float32),
        "value_weight": scatter_about(key_list[9], (D, V), D ** -0.5, 0.125, ((0, 8), (1, 4)), jnp.float32),
        "out_basis": scatter_about(key_list[10], (D, RANK), D ** -0.5, 0.125),
        "value_basis": scatter_about(key_list[11], (D, RANK), D ** -0.5, 0.125),
        "out_first": draw_out_first(jax.random.fold_in(key_list[16], 71), 0),
        "out_second": jnp.clip(jnp.exp(math.log(0.5) - 3.218876 * jax.random.uniform(key_list[13], (RANK, V), jnp.float32) ** shard_levels(key_list[13], (RANK, V), ((0, 8), (1, 4)), -0.2, 0.2)), 0.02, 0.5),
        "value_first": draw_value_first(jax.random.fold_in(key_list[16], 71), 0),
        "value_second": jnp.clip(jnp.exp(math.log(0.5) - 3.218876 * jax.random.uniform(key_list[15], (RANK, V), jnp.float32) ** shard_levels(key_list[15], (RANK, V), ((0, 8), (1, 4)), -0.2, 0.2)), 0.02, 0.5),
    }


EPSILON_NORM = 1e-05
EPSILON_ADAM = 1e-08
BETA_ONE = 0.9
BETA_TWO = 0.95
CLIP_RMS = 1.0
LEARN_RATE = 0.01

def moment_step(proj, first, second):
    new_first = BETA_ONE * first + (1.0 - BETA_ONE) * proj
    new_second = BETA_TWO * second + (1.0 - BETA_TWO) * proj * proj
    direction = new_first / (jnp.sqrt(new_second) + EPSILON_ADAM)
    return (new_first, new_second, direction)

def adapt(grad, basis, first, second):
    basis_wide = basis.astype(jnp.float32)
    proj = jnp.dot(basis_wide.T, grad, precision=lax.Precision.HIGHEST)
    new_first, new_second, direction = moment_step(proj, first, second)
    clip_factor = jnp.minimum(1.0, CLIP_RMS * math.sqrt(RANK * V) / jnp.sqrt(jnp.sum(direction * direction)))
    step_full = clip_factor * jnp.dot(basis_wide, direction, precision=lax.Precision.HIGHEST)
    return (step_full, new_first, new_second)

def reference(query_rows, key_rows, value_rows, mix_lambda, head_gain, out_cotangent, layer_input, value_cotangent, out_weight, value_weight, out_basis, value_basis, out_first, out_second, value_first, value_second):
    seq_count = TOKENS // LEN
    query_heads = query_rows.reshape(seq_count, LEN, H, 2, DH).transpose(0, 2, 3, 1, 4).reshape(seq_count * H, 2, LEN, DH)
    key_heads = key_rows.reshape(seq_count, LEN, H, 2, DH).transpose(0, 2, 3, 1, 4).reshape(seq_count * H, 2, LEN, DH)
    value_heads = value_rows.reshape(seq_count, LEN, H, DV).transpose(0, 2, 1, 3).reshape(seq_count * H, LEN, DV)
    lam_rows = jnp.tile(mix_lambda, seq_count)
    positions = jnp.arange(LEN)
    causal = positions[None, :] <= positions[:, None]

    def attend(operands):
        query_pair, key_pair, value_head, lam_value = operands
        scores = jnp.einsum('mqd,mkd->mqk', query_pair.astype(jnp.float32), key_pair.astype(jnp.float32)) * DH ** (-0.5)
        scores = jnp.where(causal[None], scores, -jnp.inf)
        row_peak = lax.optimization_barrier(jnp.max(scores, axis=-1, keepdims=True))
        exp_scores = jnp.exp(scores - row_peak)
        soft_maps = exp_scores / lax.optimization_barrier(jnp.sum(exp_scores, axis=-1, keepdims=True))
        mix_weights = (soft_maps[0] - lam_value * soft_maps[1]).astype(jnp.bfloat16)
        raw_out = jnp.dot(mix_weights, value_head, preferred_element_type=jnp.float32)
        normed = raw_out * lax.rsqrt(lax.optimization_barrier(jnp.mean(raw_out * raw_out, axis=-1, keepdims=True)) + EPSILON_NORM) * head_gain
        return normed.astype(jnp.bfloat16)
    head_blocks = lax.map(attend, (query_heads, key_heads, value_heads, lam_rows))
    head_out = head_blocks.reshape(seq_count, H, LEN, DV).transpose(0, 2, 1, 3).reshape(TOKENS, H * DV)
    out_grad = jnp.dot(out_cotangent.T, head_out, preferred_element_type=jnp.float32)
    value_grad = jnp.dot(layer_input.T, value_cotangent, preferred_element_type=jnp.float32)
    out_full, new_out_first, new_out_second = adapt(out_grad, out_basis, out_first, out_second)
    value_step, new_value_first, new_value_second = adapt(value_grad, value_basis, value_first, value_second)
    out_step = out_full.T
    new_out_weight = out_weight - LEARN_RATE * out_step
    new_value_weight = value_weight - LEARN_RATE * value_step
    return (out_step, value_step, new_out_weight, new_value_weight, new_out_weight.astype(jnp.bfloat16), new_value_weight.astype(jnp.bfloat16), new_out_first, new_out_second, new_value_first, new_value_second)
```

```python
import functools
import math

import jax
import jax.numpy as jnp
from jax import lax
from jax.experimental import pallas as pl
from jax.experimental.pallas import tpu as pltpu
from jax.sharding import PartitionSpec as P

DH = 64
DV = 128


EPSILON_NORM = 1e-05
EPSILON_ADAM = 1e-08
BETA_ONE = 0.9
BETA_TWO = 0.95
CLIP_RMS = 1.0
LEARN_RATE = 0.01
TILE = 256
F32 = jnp.float32
BF16 = jnp.bfloat16


def dot_f32(left, right, dims=((1,), (0,))):
    return lax.dot_general(left, right, (dims, ((), ())), preferred_element_type=F32)


def split_two(wide):
    high = wide.astype(BF16)
    return high, (wide - high.astype(F32)).astype(BF16)


def fold_rows(tile, op):
    rows, cols = tile.shape
    return op(tile.reshape(rows // 8, 8, cols), axis=0)


def grads_kernel(
    lam_ref, query_ref, key_ref, value_ref, gain_ref, cot_ref, input_ref, vcot_ref,
    obasis_ref, vbasis_ref, oproj_ref, vproj_ref,
    score_one, score_two, mix_ref, value_t, obasis_t, vbasis_t, cb_high, cb_low,
):
    block = pl.program_id(0)
    head = pl.program_id(1)
    span = query_ref.shape[0]
    seq_len = key_ref.shape[0]

    @pl.when((block == 0) & (head == 0))
    def _():
        obasis_t[...] = obasis_ref[...].T
        vbasis_t[...] = vbasis_ref[...].T
        oproj_ref[...] = jnp.zeros_like(oproj_ref)
        vproj_ref[...] = jnp.zeros_like(vproj_ref)

    @pl.when(block == 0)
    def _():
        value_t[head] = value_ref[:, pl.ds(pl.multiple_of(head * DV, DV), DV)].T

    @pl.when(head == 0)
    def _():
        cb = dot_f32(obasis_t[...], cot_ref[...], ((1,), (1,)))
        high, low = split_two(cb)
        cb_high[...] = high
        cb_low[...] = low
        high, low = split_two(dot_f32(vbasis_t[...], input_ref[...], ((1,), (1,))))
        vcot = vcot_ref[...]
        vproj_ref[...] += dot_f32(high, vcot) + dot_f32(low, vcot)

    columns = pl.ds(pl.multiple_of(head * DV, DV), DV)
    lam = lam_ref[head]
    lane = lax.broadcasted_iota(jnp.int32, (span, DV), 1)
    query = query_ref[:, columns].astype(F32) * DH ** (-0.5)
    query_one = jnp.where(lane < DH, query, 0.0).astype(BF16)
    query_two = jnp.where(lane < DH, 0.0, query).astype(BF16)

    def attend(width, open_from):
        def tiles():
            return range(0, width, TILE)

        peak_one = jnp.full((8, span), -jnp.inf, F32)
        peak_two = peak_one
        for at in tiles():
            keys = key_ref[at : at + TILE, columns]
            one = dot_f32(keys, query_one, ((1,), (1,)))
            two = dot_f32(keys, query_two, ((1,), (1,)))
            if at >= open_from:
                key_pos = at + lax.broadcasted_iota(jnp.int32, (TILE, span), 0)
                query_pos = block * span + lax.broadcasted_iota(jnp.int32, (TILE, span), 1)
                causal = key_pos <= query_pos
                one = jnp.where(causal, one, -jnp.inf)
                two = jnp.where(causal, two, -jnp.inf)
            score_one[at : at + TILE, :] = one
            score_two[at : at + TILE, :] = two
            peak_one = jnp.maximum(peak_one, fold_rows(one, jnp.max))
            peak_two = jnp.maximum(peak_two, fold_rows(two, jnp.max))
        peak_one = jnp.max(peak_one, axis=0, keepdims=True)
        peak_two = jnp.max(peak_two, axis=0, keepdims=True)
        sum_one = jnp.zeros((8, span), F32)
        sum_two = sum_one
        for at in tiles():
            one = jnp.exp(score_one[at : at + TILE, :] - peak_one)
            two = jnp.exp(score_two[at : at + TILE, :] - peak_two)
            score_one[at : at + TILE, :] = one
            score_two[at : at + TILE, :] = two
            sum_one += fold_rows(one, jnp.sum)
            sum_two += fold_rows(two, jnp.sum)
        rate_one = 1.0 / jnp.sum(sum_one, axis=0, keepdims=True)
        rate_two = lam / jnp.sum(sum_two, axis=0, keepdims=True)
        for at in tiles():
            mix_ref[at : at + TILE, :] = (
                score_one[at : at + TILE, :] * rate_one - score_two[at : at + TILE, :] * rate_two
            ).astype(BF16)
        raw = dot_f32(value_t[head, :, :width], mix_ref[:width, :])
        mean_sq = jnp.mean(raw * raw, axis=0, keepdims=True)
        out_t = (raw * lax.rsqrt(mean_sq + EPSILON_NORM) * gain_ref[...]).astype(BF16)
        oproj_ref[:, columns] += dot_f32(cb_high[...], out_t, ((1,), (1,))) + dot_f32(
            cb_low[...], out_t, ((1,), (1,))
        )

    step = min(2 * span, seq_len)
    for width in range(step, seq_len + 1, step):
        lowest = (width - step) // span

        @pl.when((block >= lowest) & (block < width // span))
        def _(width=width):
            attend(width, width - step)


def local_grads(
    query_rows, key_rows, value_rows, mix_lambda, head_gain, out_cotangent, layer_input,
    value_cotangent, out_basis, value_basis,
):
    seq_len, cols = query_rows.shape
    heads = mix_lambda.shape[0]
    width = out_cotangent.shape[1]
    rank = out_basis.shape[1]
    span = min(TILE, seq_len)
    blocks = seq_len // span
    rows_spec = lambda wide: pl.BlockSpec((span, wide), lambda i, h: (i, 0))
    whole = lambda a, b: pl.BlockSpec((a, b), lambda i, h: (0, 0))
    return pl.pallas_call(
        grads_kernel,
        grid=(blocks, heads),
        out_shape=(
            jax.ShapeDtypeStruct((rank, cols), F32),
            jax.ShapeDtypeStruct((rank, cols), F32),
        ),
        in_specs=[
            pl.BlockSpec(memory_space=pltpu.SMEM),
            rows_spec(cols),
            whole(seq_len, cols),
            whole(seq_len, cols),
            whole(DV, 1),
            rows_spec(width),
            rows_spec(width),
            rows_spec(cols),
            whole(width, rank),
            whole(width, rank),
        ],
        out_specs=(whole(rank, cols), whole(rank, cols)),
        scratch_shapes=[
            pltpu.VMEM((seq_len, span), F32),
            pltpu.VMEM((seq_len, span), F32),
            pltpu.VMEM((seq_len, span), BF16),
            pltpu.VMEM((heads, DV, seq_len), BF16),
            pltpu.VMEM((rank, width), BF16),
            pltpu.VMEM((rank, width), BF16),
            pltpu.VMEM((rank, span), BF16),
            pltpu.VMEM((rank, span), BF16),
        ],
        compiler_params=pltpu.CompilerParams(
            dimension_semantics=("arbitrary", "arbitrary"),
            vmem_limit_bytes=60 * 1024 * 1024,
        ),
        name="grads",
    )(
        mix_lambda, query_rows, key_rows, value_rows, head_gain.reshape(DV, 1),
        out_cotangent, layer_input, value_cotangent, out_basis, value_basis,
    )


def moment_step(proj, first, second):
    new_first = BETA_ONE * first + (1.0 - BETA_ONE) * proj
    new_second = BETA_TWO * second + (1.0 - BETA_TWO) * proj * proj
    direction = new_first / (jnp.sqrt(new_second) + EPSILON_ADAM)
    return (new_first, new_second, direction)


def body(
    query_rows,
    key_rows,
    value_rows,
    mix_lambda,
    head_gain,
    out_cotangent,
    layer_input,
    value_cotangent,
    out_weight,
    value_weight,
    out_basis,
    value_basis,
    out_first,
    out_second,
    value_first,
    value_second,
):
    fs_count = lax.axis_size("fs")
    row_share = out_cotangent.shape[1] // fs_count
    row_base = lax.axis_index("fs") * row_share
    out_rows_b = lax.dynamic_slice_in_dim(out_basis, row_base, row_share, 0).astype(jnp.float32)
    value_rows_b = lax.dynamic_slice_in_dim(value_basis, row_base, row_share, 0).astype(jnp.float32)
    out_part, value_part = local_grads(
        query_rows, key_rows, value_rows, mix_lambda, head_gain, out_cotangent, layer_input,
        value_cotangent, out_basis, value_basis,
    )
    out_proj = lax.psum_scatter(out_part, "fs", scatter_dimension=0, tiled=True)
    value_proj = lax.psum_scatter(value_part, "fs", scatter_dimension=0, tiled=True)
    new_out_first, new_out_second, out_dir = moment_step(out_proj, out_first, out_second)
    new_value_first, new_value_second, value_dir = moment_step(
        value_proj, value_first, value_second
    )
    out_sumsq, value_sumsq = lax.psum(
        (jnp.sum(out_dir * out_dir), jnp.sum(value_dir * value_dir)), ("fs", "tp")
    )
    entry_count = out_first.shape[0] * fs_count * out_first.shape[1] * lax.axis_size("tp")
    out_clip = jnp.minimum(1.0, CLIP_RMS * math.sqrt(entry_count) / jnp.sqrt(out_sumsq))
    value_clip = jnp.minimum(1.0, CLIP_RMS * math.sqrt(entry_count) / jnp.sqrt(value_sumsq))
    out_total = jnp.dot(
        out_rows_b,
        lax.all_gather(out_dir, "fs", axis=0, tiled=True),
        precision=lax.Precision.HIGHEST,
    )
    value_total = jnp.dot(
        value_rows_b,
        lax.all_gather(value_dir, "fs", axis=0, tiled=True),
        precision=lax.Precision.HIGHEST,
    )
    value_step = value_clip * value_total
    out_step = (out_clip * out_total).T
    new_value_weight = value_weight - LEARN_RATE * value_step
    new_out_weight = out_weight - LEARN_RATE * out_step
    out_copy, value_copy = (
        lax.all_gather(new_out_weight.astype(jnp.bfloat16), "fs", axis=1, tiled=True),
        lax.all_gather(new_value_weight.astype(jnp.bfloat16), "fs", axis=0, tiled=True),
    )
    return (
        out_step,
        value_step,
        new_out_weight,
        new_value_weight,
        out_copy,
        value_copy,
        new_out_first,
        new_out_second,
        new_value_first,
        new_value_second,
    )


def solution(mesh):
    placed = (
        P("fs", "tp"),
        P("fs", "tp"),
        P("fs", "tp"),
        P("tp"),
        P(),
        P("fs", None),
        P("fs", None),
        P("fs", "tp"),
        P("tp", "fs"),
        P("fs", "tp"),
        P(),
        P(),
        P("fs", "tp"),
        P("fs", "tp"),
        P("fs", "tp"),
        P("fs", "tp"),
    )
    return jax.shard_map(
        body,
        mesh=mesh,
        in_specs=placed,
        out_specs=(
            P("tp", "fs"),
            P("fs", "tp"),
            P("tp", "fs"),
            P("fs", "tp"),
            P("tp", None),
            P(None, "tp"),
            P("fs", "tp"),
            P("fs", "tp"),
            P("fs", "tp"),
            P("fs", "tp"),
        ),
        check_vma=False,
    )
```

```python
import functools
import math

import jax
import jax.numpy as jnp
from jax import lax
from jax.experimental import pallas as pl
from jax.experimental.pallas import tpu as pltpu
from jax.sharding import PartitionSpec as P

DH = 64
DV = 128


EPSILON_NORM = 1e-05
EPSILON_ADAM = 1e-08
BETA_ONE = 0.9
BETA_TWO = 0.95
CLIP_RMS = 1.0
LEARN_RATE = 0.01
TILE = 256
F32 = jnp.float32
BF16 = jnp.bfloat16


def dot_f32(left, right, dims=((1,), (0,))):
    return lax.dot_general(left, right, (dims, ((), ())), preferred_element_type=F32)


def split_two(wide):
    high = wide.astype(BF16)
    return high, (wide - high.astype(F32)).astype(BF16)


def fold_rows(tile, op):
    rows, cols = tile.shape
    return op(tile.reshape(rows // 8, 8, cols), axis=0)


def grads_kernel(
    lam_ref, query_ref, key_ref, value_ref, gain_ref, cot_ref, input_ref, vcot_ref,
    obasis_ref, vbasis_ref, oproj_ref, vproj_ref,
    score_one, score_two, mix_ref, value_t, obasis_t, vbasis_t, cb_high, cb_low,
):
    block = pl.program_id(0)
    head = pl.program_id(1)
    span = query_ref.shape[0]
    seq_len = key_ref.shape[0]

    @pl.when((block == 0) & (head == 0))
    def _():
        obasis_t[...] = obasis_ref[...].T
        vbasis_t[...] = vbasis_ref[...].T
        oproj_ref[...] = jnp.zeros_like(oproj_ref)
        vproj_ref[...] = jnp.zeros_like(vproj_ref)

    @pl.when(block == 0)
    def _():
        value_t[head] = value_ref[:, pl.ds(pl.multiple_of(head * DV, DV), DV)].T

    @pl.when(head == 0)
    def _():
        cb = dot_f32(obasis_t[...], cot_ref[...], ((1,), (1,)))
        high, low = split_two(cb)
        cb_high[...] = high
        cb_low[...] = low
        high, low = split_two(dot_f32(vbasis_t[...], input_ref[...], ((1,), (1,))))
        vcot = vcot_ref[...]
        vproj_ref[...] += dot_f32(high, vcot) + dot_f32(low, vcot)

    columns = pl.ds(pl.multiple_of(head * DV, DV), DV)
    lam = lam_ref[head]
    lane = lax.broadcasted_iota(jnp.int32, (span, DV), 1)
    query = query_ref[:, columns].astype(F32) * DH ** (-0.5)
    query_one = jnp.where(lane < DH, query, 0.0).astype(BF16)
    query_two = jnp.where(lane < DH, 0.0, query).astype(BF16)

    def attend(width, open_from):
        def tiles():
            return range(0, width, TILE)

        peak_one = jnp.full((8, span), -jnp.inf, F32)
        peak_two = peak_one
        for at in tiles():
            keys = key_ref[at : at + TILE, columns]
            one = dot_f32(keys, query_one, ((1,), (1,)))
            two = dot_f32(keys, query_two, ((1,), (1,)))
            if at >= open_from:
                key_pos = at + lax.broadcasted_iota(jnp.int32, (TILE, span), 0)
                query_pos = block * span + lax.broadcasted_iota(jnp.int32, (TILE, span), 1)
                causal = key_pos <= query_pos
                one = jnp.where(causal, one, -jnp.inf)
                two = jnp.where(causal, two, -jnp.inf)
            score_one[at : at + TILE, :] = one
            score_two[at : at + TILE, :] = two
            peak_one = jnp.maximum(peak_one, fold_rows(one, jnp.max))
            peak_two = jnp.maximum(peak_two, fold_rows(two, jnp.max))
        peak_one = jnp.max(peak_one, axis=0, keepdims=True)
        peak_two = jnp.max(peak_two, axis=0, keepdims=True)
        sum_one = jnp.zeros((8, span), F32)
        sum_two = sum_one
        for at in tiles():
            one = jnp.exp(score_one[at : at + TILE, :] - peak_one)
            two = jnp.exp(score_two[at : at + TILE, :] - peak_two)
            score_one[at : at + TILE, :] = one
            score_two[at : at + TILE, :] = two
            sum_one += fold_rows(one, jnp.sum)
            sum_two += fold_rows(two, jnp.sum)
        rate_one = 1.0 / jnp.sum(sum_one, axis=0, keepdims=True)
        rate_two = lam / jnp.sum(sum_two, axis=0, keepdims=True)
        for at in tiles():
            mix_ref[at : at + TILE, :] = (
                score_one[at : at + TILE, :] * rate_one - score_two[at : at + TILE, :] * rate_two
            ).astype(BF16)
        raw = dot_f32(value_t[head, :, :width], mix_ref[:width, :])
        mean_sq = jnp.mean(raw * raw, axis=0, keepdims=True)
        out_t = (raw * lax.rsqrt(mean_sq + EPSILON_NORM) * gain_ref[...]).astype(BF16)
        oproj_ref[:, columns] += dot_f32(cb_high[...], out_t, ((1,), (1,))) + dot_f32(
            cb_low[...], out_t, ((1,), (1,))
        )

    step = min(2 * span, seq_len)
    for width in range(step, seq_len + 1, step):
        lowest = (width - step) // span

        @pl.when((block >= lowest) & (block < width // span))
        def _(width=width):
            attend(width, width - step)


def local_grads(
    query_rows, key_rows, value_rows, mix_lambda, head_gain, out_cotangent, layer_input,
    value_cotangent, out_basis, value_basis,
):
    seq_len, cols = query_rows.shape
    heads = mix_lambda.shape[0]
    width = out_cotangent.shape[1]
    rank = out_basis.shape[1]
    span = min(TILE, seq_len)
    blocks = seq_len // span
    rows_spec = lambda wide: pl.BlockSpec((span, wide), lambda i, h: (i, 0))
    whole = lambda a, b: pl.BlockSpec((a, b), lambda i, h: (0, 0))
    return pl.pallas_call(
        grads_kernel,
        grid=(blocks, heads),
        out_shape=(
            jax.ShapeDtypeStruct((rank, cols), F32),
            jax.ShapeDtypeStruct((rank, cols), F32),
        ),
        in_specs=[
            pl.BlockSpec(memory_space=pltpu.SMEM),
            rows_spec(cols),
            whole(seq_len, cols),
            whole(seq_len, cols),
            whole(DV, 1),
            rows_spec(width),
            rows_spec(width),
            rows_spec(cols),
            whole(width, rank),
            whole(width, rank),
        ],
        out_specs=(whole(rank, cols), whole(rank, cols)),
        scratch_shapes=[
            pltpu.VMEM((seq_len, span), F32),
            pltpu.VMEM((seq_len, span), F32),
            pltpu.VMEM((seq_len, span), BF16),
            pltpu.VMEM((heads, DV, seq_len), BF16),
            pltpu.VMEM((rank, width), BF16),
            pltpu.VMEM((rank, width), BF16),
            pltpu.VMEM((rank, span), BF16),
            pltpu.VMEM((rank, span), BF16),
        ],
        compiler_params=pltpu.CompilerParams(
            dimension_semantics=("arbitrary", "arbitrary"),
            vmem_limit_bytes=60 * 1024 * 1024,
        ),
        name="grads",
    )(
        mix_lambda, query_rows, key_rows, value_rows, head_gain.reshape(DV, 1),
        out_cotangent, layer_input, value_cotangent, out_basis, value_basis,
    )


def moment_step(proj, first, second):
    new_first = BETA_ONE * first + (1.0 - BETA_ONE) * proj
    new_second = BETA_TWO * second + (1.0 - BETA_TWO) * proj * proj
    direction = new_first / (jnp.sqrt(new_second) + EPSILON_ADAM)
    return (new_first, new_second, direction)


def finish_kernel(
    fs_count, tp_count,
    opart, vpart, ofirst, osecond, vfirst, vsecond, obasis, vbasis, oweight, vweight,
    ostep, vstep, onew, vnew, ocopy, vcopy, ofirst_new, osecond_new, vfirst_new, vsecond_new,
    got, dirs, squares, squares_got,
    scatter_send, scatter_recv, ring_send, ring_recv, copy_send, copy_recv, sq_send, sq_recv,
):
    me = lax.axis_index("fs")
    my_tp = lax.axis_index("tp")
    half_count = fs_count // 2
    rank_share = ofirst.shape[0]
    cols = ofirst.shape[1]
    row_share = vweight.shape[0]
    mesh_ids = pl.DeviceIdType.MESH

    place = jnp.where(me % 2 == 0, me // 2, fs_count - 1 - me // 2)

    def owner(at):
        at = lax.rem(at + 2 * fs_count, fs_count)
        return jnp.where(at < half_count, 2 * at, 2 * (fs_count - 1 - at) + 1)

    def fs_peer(gap):
        return lax.rem(me + gap, fs_count)

    def tp_peer(gap):
        return lax.rem(my_tp + gap, tp_count)

    barrier = pltpu.get_barrier_semaphore()
    for gap in range(1, fs_count):
        pl.semaphore_signal(
            barrier, inc=1, device_id=(fs_peer(gap), my_tp), device_id_type=mesh_ids
        )
    for gap in range(1, tp_count):
        pl.semaphore_signal(
            barrier, inc=1, device_id=(me, tp_peer(gap)), device_id_type=mesh_ids
        )
    pl.semaphore_wait(barrier, fs_count + tp_count - 2)

    def share(index, size):
        return pl.ds(pl.multiple_of(index * size, size), size)

    parts = (vpart, opart)
    scatters = ([], [])
    for mat in range(2):
        for gap in range(1, fs_count):
            peer = fs_peer(gap)
            copy = pltpu.make_async_remote_copy(
                src_ref=parts[mat].at[share(peer, rank_share)],
                dst_ref=got.at[mat, gap - 1],
                send_sem=scatter_send.at[mat, gap - 1],
                recv_sem=scatter_recv.at[mat, gap - 1],
                device_id=(peer, my_tp),
                device_id_type=mesh_ids,
            )
            copy.start()
            scatters[mat].append(copy)

    def ring(blocks, sems_send, sems_recv):
        def make(mat, step, way):
            origin = owner(place - step if way == 0 else place + step)
            split = way if step == half_count - 1 else None
            ref = blocks[mat](origin, split)
            target = owner(place + 1 if way == 0 else place - 1)
            return pltpu.make_async_remote_copy(
                src_ref=ref,
                dst_ref=ref,
                send_sem=sems_send.at[mat, way, step],
                recv_sem=sems_recv.at[mat, way, step],
                device_id=(target, my_tp),
                device_id_type=mesh_ids,
            )

        def arrival(mat, step, way):
            origin = owner(place - 1 - step if way == 0 else place + 1 + step)
            split = way if step == half_count - 1 else None
            ref = blocks[mat](origin, split)
            return pltpu.make_async_remote_copy(
                src_ref=ref,
                dst_ref=ref,
                send_sem=sems_send.at[mat, way, step],
                recv_sem=sems_recv.at[mat, way, step],
                device_id=(owner(place + 1), my_tp),
                device_id_type=mesh_ids,
            )

        started = []

        def begin(mat):
            for way in range(2):
                copy = make(mat, 0, way)
                copy.start()
                started.append(copy)

        def drain():
            for step in range(half_count):
                for mat in range(len(blocks)):
                    for way in range(2):
                        arrival(mat, step, way).wait_recv()
                        if step + 1 < half_count:
                            copy = make(mat, step + 1, way)
                            copy.start()
                            started.append(copy)
            for copy in started:
                copy.wait_send()

        return begin, drain

    def halved(start, size, split):
        if split is None:
            return pl.ds(pl.multiple_of(start, size), size)
        return pl.ds(pl.multiple_of(start + split * (size // 2), size // 2), size // 2)

    begin, drain = ring(
        [
            lambda at, split, mat=mat: dirs.at[mat, halved(at * rank_share, rank_share, split)]
            for mat in range(2)
        ],
        ring_send, ring_recv,
    )
    moments = (
        (vfirst, vsecond, vfirst_new, vsecond_new),
        (ofirst, osecond, ofirst_new, osecond_new),
    )
    for mat in range(2):
        proj = parts[mat][share(me, rank_share), :]
        for gap in range(1, fs_count):
            scatters[mat][gap - 1].wait_recv()
            proj += got[mat, gap - 1]
        first, second, first_new, second_new = moments[mat]
        new_first, new_second, direction = moment_step(proj, first[...], second[...])
        dirs[mat, share(me, rank_share), :] = direction
        begin(mat)
        first_new[...] = new_first
        second_new[...] = new_second
    drain()

    for mat in range(2):
        whole = dirs[mat]
        squared = fold_rows(whole * whole, jnp.sum)
        total = squared[:, :128]
        for at in range(128, cols, 128):
            total += squared[:, at : at + 128]
        squares[mat] = total
    exchanges = []
    for gap in range(1, tp_count):
        copy = pltpu.make_async_remote_copy(
            src_ref=squares,
            dst_ref=squares_got.at[gap - 1],
            send_sem=sq_send.at[gap - 1],
            recv_sem=sq_recv.at[gap - 1],
            device_id=(me, tp_peer(gap)),
            device_id_type=mesh_ids,
        )
        copy.start()
        exchanges.append(copy)

    high, low = split_two(dirs[0])
    vstep[...] = dot_f32(vbasis[...], high) + dot_f32(vbasis[...], low)
    high, low = split_two(dirs[1])
    ostep[...] = dot_f32(high, obasis[...], ((0,), (1,))) + dot_f32(
        low, obasis[...], ((0,), (1,))
    )
    for copy in exchanges:
        copy.wait_recv()
    entry_count = rank_share * fs_count * cols * tp_count

    def clip_of(mat):
        total = squares[mat]
        for gap in range(1, tp_count):
            total += squares_got[gap - 1, mat]
        total = jnp.sum(jnp.sum(total, axis=0, keepdims=True), axis=1, keepdims=True)
        return jnp.minimum(1.0, CLIP_RMS * math.sqrt(entry_count) / jnp.sqrt(total))

    begin, drain = ring(
        [
            lambda at, split: vcopy.at[halved(at * row_share, row_share, split)],
            lambda at, split: ocopy.at[
                slice(None) if split is None else pl.ds(split * (cols // 2), cols // 2),
                share(at, row_share),
            ],
        ],
        copy_send, copy_recv,
    )
    step = clip_of(0) * vstep[...]
    vstep[...] = step
    weight = vweight[...] - LEARN_RATE * step
    vnew[...] = weight
    vcopy[share(me, row_share), :] = weight.astype(BF16)
    begin(0)
    step = clip_of(1) * ostep[...]
    ostep[...] = step
    weight = oweight[...] - LEARN_RATE * step
    onew[...] = weight
    ocopy[:, share(me, row_share)] = weight.astype(BF16)
    begin(1)
    drain()
    for copy in scatters[0] + scatters[1] + exchanges:
        copy.wait_send()


def finish(
    out_part, value_part, out_first, out_second, value_first, value_second, out_rows_b,
    value_rows_b, out_weight, value_weight,
):
    fs_count = lax.axis_size("fs")
    tp_count = lax.axis_size("tp")
    rank, cols = out_part.shape
    row_share = value_weight.shape[0]
    like = lambda a: jax.ShapeDtypeStruct(a.shape, a.dtype)
    half_count = fs_count // 2
    dma = pltpu.SemaphoreType.DMA
    return pl.pallas_call(
        functools.partial(finish_kernel, fs_count, tp_count),
        out_shape=(
            like(out_weight), like(value_weight), like(out_weight), like(value_weight),
            jax.ShapeDtypeStruct((cols, row_share * fs_count), BF16),
            jax.ShapeDtypeStruct((row_share * fs_count, cols), BF16),
            like(out_first), like(out_second), like(value_first), like(value_second),
        ),
        in_specs=[pl.BlockSpec(memory_space=pltpu.VMEM)] * 10,
        out_specs=tuple([pl.BlockSpec(memory_space=pltpu.VMEM)] * 10),
        scratch_shapes=[
            pltpu.VMEM((2, fs_count - 1, rank // fs_count, cols), F32),
            pltpu.VMEM((2, rank, cols), F32),
            pltpu.VMEM((2, 8, 128), F32),
            pltpu.VMEM((tp_count - 1, 2, 8, 128), F32),
            dma((2, fs_count - 1)), dma((2, fs_count - 1)),
            dma((2, 2, half_count)), dma((2, 2, half_count)),
            dma((2, 2, half_count)), dma((2, 2, half_count)),
            dma((tp_count - 1,)), dma((tp_count - 1,)),
        ],
        compiler_params=pltpu.CompilerParams(
            collective_id=0, has_side_effects=True, vmem_limit_bytes=48 * 1024 * 1024
        ),
        name="finish",
    )(
        out_part, value_part, out_first, out_second, value_first, value_second, out_rows_b,
        value_rows_b, out_weight, value_weight,
    )


def body(
    query_rows, key_rows, value_rows, mix_lambda, head_gain, out_cotangent, layer_input,
    value_cotangent, out_weight, value_weight, out_basis, value_basis, out_first, out_second,
    value_first, value_second,
):
    row_share = out_cotangent.shape[1] // lax.axis_size("fs")
    row_base = lax.axis_index("fs") * row_share
    out_rows_b = lax.dynamic_slice_in_dim(out_basis, row_base, row_share, 0)
    value_rows_b = lax.dynamic_slice_in_dim(value_basis, row_base, row_share, 0)
    out_part, value_part = local_grads(
        query_rows, key_rows, value_rows, mix_lambda, head_gain, out_cotangent, layer_input,
        value_cotangent, out_basis, value_basis,
    )
    return finish(
        out_part, value_part, out_first, out_second, value_first, value_second, out_rows_b,
        value_rows_b, out_weight, value_weight,
    )


def solution(mesh):
    placed = (
        P("fs", "tp"),
        P("fs", "tp"),
        P("fs", "tp"),
        P("tp"),
        P(),
        P("fs", None),
        P("fs", None),
        P("fs", "tp"),
        P("tp", "fs"),
        P("fs", "tp"),
        P(),
        P(),
        P("fs", "tp"),
        P("fs", "tp"),
        P("fs", "tp"),
        P("fs", "tp"),
    )
    return jax.shard_map(
        body,
        mesh=mesh,
        in_specs=placed,
        out_specs=(
            P("tp", "fs"),
            P("fs", "tp"),
            P("tp", "fs"),
            P("fs", "tp"),
            P("tp", None),
            P(None, "tp"),
            P("fs", "tp"),
            P("fs", "tp"),
            P("fs", "tp"),
            P("fs", "tp"),
        ),
        check_vma=False,
    )
```
